128 devices in a mesh: rep: 2 (over z_hi), fs: 32 (over z_lo, y, x), tp: 2 (over core).
Axes of the slice: x: 4, y: 4, z: 4 (z_hi: 2, z_lo: 2; z = z_hi * 2 + z_lo), core: 2. Of those that a mesh axis runs over, the one named last changes fastest.
Arguments:
- tokens: bfloat16 [64, 256, 1024], P(('rep', 'fs'), None, 'tp'), may hold values from -6 to 6
- pre_gain: float32 [1024], replicated, may hold values from 0.1 to 1.9
- first_gate: bfloat16 [1024, 2560], P('fs', 'tp'), may hold values from -0.1875 to 0.1875
- first_up: bfloat16 [1024, 2560], P('fs', 'tp'), may hold values from -0.1875 to 0.1875
- first_down: bfloat16 [2560, 1024], P('tp', 'fs'), may hold values from -0.125 to 0.125
- mix_gain: float32 [1024], P('tp'), may hold values from 0.1 to 1.9
- pool_weight: bfloat16 [4, 256, 256], P('tp', None, 'fs'), may hold values from -0.375 to 0.375
- pool_scale: float32 [1024], P('tp'), may hold values from 0.1 to 1.9
- post_gain: float32 [1024], replicated, may hold values from 0.1 to 1.9
- second_gate: bfloat16 [1024, 2560], P('fs', 'tp'), may hold values from -0.1875 to 0.1875
- second_up: bfloat16 [1024, 2560], P('fs', 'tp'), may hold values from -0.1875 to 0.1875
- second_down: bfloat16 [2560, 1024], P('tp', 'fs'), may hold values from -0.125 to 0.125
Outputs:
- layer_out: bfloat16 [64, 256, 1024], P(('rep', 'fs'), None, 'tp')
The draws below stay inside these ranges and needn't reach their ends.
All inputs are finite; a program needn't handle non-finite values.
Results may differ from the reference program's by a relative error of at most 0.015.
Values may be sent and summed in bfloat16 or wider, within the bound.
No kernel may reach another device: no remote copies, remote signals or barrier semaphores. Data moves between devices by JAX's collectives and lax.ppermute only.
A program may use at most 64 MiB of HBM per device.

```python
import jax
import jax.numpy as jnp
from jax import lax

D = 1024
FF = 2560
GROUPS = 4
GROUP = 256
SEQ = 256
BATCH = 64


def levels(stream_key, extent, cuts, least, high):
    loudness = 1.0
    for axis_at, shards_of in cuts:
        steps = jax.random.uniform(jax.random.fold_in(jax.random.fold_in(stream_key, 6), axis_at), (shards_of,), jnp.float32, least / len(cuts), high / len(cuts))
        loudness = loudness * jnp.repeat(jnp.exp(steps), extent[axis_at] // shards_of).reshape((-1,) + (1,) * (len(extent) - 1 - axis_at))
    return loudness


def scatter_about(own_key, shape, deviation, reach, shards=(), held_as=jnp.bfloat16):
    values = deviation * jax.random.normal(own_key, shape, jnp.float32)
    if shards:
        values = values * levels(own_key, shape, shards, -0.22, 0.18)
    return jnp.clip(values, -reach, reach).astype(held_as)


def setup_inputs(seed: int = 0) -> dict:
    key_of = jax.random.split(jax.random.key(seed), 13)
    tokens = scatter_about(key_of[0], (BATCH, SEQ, D), 1.0, 6.0, ((0, 64), (2, 2)))
    pre_gain = jnp.clip(1.0 + 0.18 * jax.random.normal(key_of[1], (D,), jnp.float32), 0.1, 1.9)
    first_gate = scatter_about(key_of[2], (D, FF), D ** -0.5, 0.1875, ((0, 32), (1, 2)))
    first_up = scatter_about(key_of[3], (D, FF), D ** -0.5, 0.1875, ((0, 32), (1, 2)))
    first_down = scatter_about(key_of[4], (FF, D), FF ** -0.5, 0.125, ((0, 2), (1, 32)))
    mix_gain = jnp.clip(1.0 + 0.18 * jax.random.normal(key_of[5], (D,), jnp.float32), 0.1, 1.9)
    pool_weight = scatter_about(key_of[6], (GROUPS, GROUP, GROUP), GROUP ** -0.5, 0.375, ((0, 2), (2, 32)))
    pool_scale = jnp.clip(1.0 + 0.18 * jax.random.normal(key_of[7], (D,), jnp.float32), 0.1, 1.9)
    post_gain = jnp.clip(1.0 + 0.18 * jax.random.normal(key_of[8], (D,), jnp.float32), 0.1, 1.9)
    second_gate = scatter_about(key_of[9], (D, FF), D ** -0.5, 0.1875, ((0, 32), (1, 2)))
    second_up = scatter_about(key_of[10], (D, FF), D ** -0.5, 0.1875, ((0, 32), (1, 2)))
    second_down = scatter_about(key_of[11], (FF, D), FF ** -0.5, 0.125, ((0, 2), (1, 32)))
    return dict(tokens=tokens, pre_gain=pre_gain, first_gate=first_gate, first_up=first_up, first_down=first_down, mix_gain=mix_gain, pool_weight=pool_weight, pool_scale=pool_scale, post_gain=post_gain, second_gate=second_gate, second_up=second_up, second_down=second_down)


epsilon = 1e-06

def normalize(values, gain_vec):
    floats = values.astype(jnp.float32)
    scaled = floats * lax.rsqrt(lax.optimization_barrier(jnp.mean(floats * floats, axis=-1, keepdims=True)) + epsilon)
    return (scaled * gain_vec.astype(jnp.float32)).astype(jnp.bfloat16)

def half_block(flat_rows, gain_vec, gate_w, up_w, down_w):
    normed = normalize(flat_rows, gain_vec)
    gate_sum = jnp.dot(normed, gate_w, preferred_element_type=jnp.float32)
    up_sum = jnp.dot(normed, up_w, preferred_element_type=jnp.float32)
    hidden = (jax.nn.silu(gate_sum) * up_sum).astype(jnp.bfloat16)
    return jnp.dot(hidden, down_w, preferred_element_type=jnp.float32)

def trailing(grouped, windows, widest):
    seq_length = grouped.shape[1]
    running = jnp.zeros_like(grouped)
    for back_step in range(widest):
        moved = jnp.pad(grouped, ((0, 0), (back_step, 0), (0, 0), (0, 0)))[:, :seq_length]
        running = running + jnp.where(back_step < windows[None, None, :, None], moved, 0.0)
    positions = jnp.arange(seq_length, dtype=jnp.int32)
    counts = jnp.minimum(positions[:, None] + 1, windows[None, :]).astype(jnp.float32)
    return running / counts[None, :, :, None]

def reference(tokens, pre_gain, first_gate, first_up, first_down, mix_gain, pool_weight, pool_scale, post_gain, second_gate, second_up, second_down):
    flat_rows = tokens.reshape(BATCH * SEQ, D)
    first_out = half_block(flat_rows, pre_gain, first_gate, first_up, first_down)
    after_first = (flat_rows.astype(jnp.float32) + 0.5 * first_out).astype(jnp.bfloat16)
    normed = normalize(after_first, mix_gain)
    grouped = normed.astype(jnp.float32).reshape(BATCH, SEQ, GROUPS, GROUP)
    windows = 2 ** (jnp.arange(GROUPS, dtype=jnp.int32) + 1)
    pooled = trailing(grouped, windows, 2 ** GROUPS)
    diff = (pooled - grouped).astype(jnp.bfloat16)
    mixed = jnp.einsum('bsgc,gcd->bsgd', diff.astype(jnp.float32), pool_weight.astype(jnp.float32))
    mixed = mixed.reshape(BATCH * SEQ, D)
    after_mix = (after_first.astype(jnp.float32) + mixed * pool_scale.astype(jnp.float32)).astype(jnp.bfloat16)
    second_out = half_block(after_mix, post_gain, second_gate, second_up, second_down)
    layer_out = (after_mix.astype(jnp.float32) + 0.5 * second_out).astype(jnp.bfloat16)
    return layer_out.reshape(BATCH, SEQ, D)
```

```python
import functools

import jax
import jax.numpy as jnp
from jax import lax
from jax.experimental import pallas as pl
from jax.experimental.pallas import tpu as pltpu
from jax.sharding import Mesh, PartitionSpec as P

EPS = 1e-06
Z = ("zh", "zl")
D = 1024
HALF = D // 2
SEQ = 256
SHARD = 32
KEEP = 640
POOL_ROWS = 8
VMEM = pl.BlockSpec(memory_space=pltpu.VMEM)
SMEM = pl.BlockSpec(memory_space=pltpu.SMEM)


def swap(value, axis, mask, size=4):
    return lax.ppermute(value, axis, [(i, i ^ mask) for i in range(size)])


def across(value):
    return swap(value, "c", 1, 2)


def after(value, *others):
    return lax.optimization_barrier((value,) + others)[0]


def near(piece, axis):
    return jnp.stack([piece] + [swap(piece, axis, m) for m in (1, 2, 3)])


def wide(block, axis):
    one = swap(block, axis, 1)
    three = swap(block, axis, 3)
    far_a = swap(three[:2], axis, 1)
    far_b = swap(one[2:], axis, 3)
    return block, one, far_a, far_b, three


def gather(own, other):
    a1 = near(own, "x")
    b1 = near(other, "y")
    a1, b1 = lax.optimization_barrier((a1, b1))
    return wide(a1, "y") + wide(b1, "x")


def pack(gate, up, down, half, pool=None):
    rows = [
        lax.dynamic_slice_in_dim(gate, half * KEEP, KEEP, 1),
        lax.dynamic_slice_in_dim(up, half * KEEP, KEEP, 1),
        lax.dynamic_slice_in_dim(down, half * KEEP, KEEP, 0).T,
    ]
    if pool is not None:
        rows.append(pool)
    return jnp.concatenate(rows, axis=0)


def ffn_kernel(with_pool, where, own0, own1, oth0, oth1, gain, *refs):
    pieces, refs = refs[:10], refs[10:]
    if with_pool:
        keep, send, pool_out, wg, wu, wd, norm = refs
    else:
        keep, send, wg, wu, wd, norm = refs
    zl, y, x, c = where[0], where[1], where[2], where[3]
    for side in range(2):
        row_half = zl if side == 0 else 1 - zl
        base = jnp.bitwise_xor(row_half, c)
        for j, ref in zip((0, 1, (2, 0), (2, 2), 3), pieces[5 * side : 5 * side + 5]):
            j, first = j if isinstance(j, tuple) else (j, 0)
            for i in range(ref.shape[0]):
                k = first + i
                if side == 0:
                    yy, xx = jnp.bitwise_xor(y, j), jnp.bitwise_xor(x, k)
                else:
                    yy, xx = jnp.bitwise_xor(y, k), jnp.bitwise_xor(x, j)
                shard = yy * 4 + xx
                at = pl.ds(pl.multiple_of((base * 16 + shard) * SHARD, SHARD), SHARD)
                wg[at, :] = ref[i, 0:SHARD, :]
                wu[at, :] = ref[i, SHARD : 2 * SHARD, :]
                wd[at, :] = ref[i, 2 * SHARD : 3 * SHARD, :]
                if with_pool:
                    spot = pl.ds(pl.multiple_of((row_half * 16 + shard) * POOL_ROWS, POOL_ROWS), POOL_ROWS)
                    pool_out[spot, :] = ref[i, 3 * SHARD :, :HALF].astype(jnp.float32)
    gain_own = gain[pl.ds(c, 1), :]
    gain_oth = gain[pl.ds(1 - c, 1), :]
    for row, (own, oth) in enumerate(((own0, oth0), (own1, oth1))):
        a = own[...].astype(jnp.float32)
        b = oth[...].astype(jnp.float32)
        total = jnp.sum(a * a + b * b, axis=1, keepdims=True)
        scale = lax.rsqrt(total / D + EPS)
        span = pl.ds(row * SEQ, SEQ)
        norm[span, :HALF] = (a * scale * gain_own).astype(jnp.bfloat16)
        norm[span, HALF:] = (b * scale * gain_oth).astype(jnp.bfloat16)
    gate = jnp.dot(norm[...], wg[...], preferred_element_type=jnp.float32)
    up = jnp.dot(norm[...], wu[...], preferred_element_type=jnp.float32)
    hidden = (gate * jax.nn.sigmoid(gate) * up).astype(jnp.bfloat16)
    out = lax.dot_general(
        hidden, wd[...], (((1,), (1,)), ((), ())), preferred_element_type=jnp.float32
    )
    keep[...] = out[:, :HALF]
    send[...] = out[:, HALF:].astype(jnp.bfloat16)


def ffn(where, own0, own1, oth0, oth1, gain, pieces, with_pool):
    out = [
        jax.ShapeDtypeStruct((2 * SEQ, HALF), jnp.float32),
        jax.ShapeDtypeStruct((2 * SEQ, HALF), jnp.bfloat16),
    ]
    if with_pool:
        out.append(jax.ShapeDtypeStruct((256, HALF), jnp.float32))
    return pl.pallas_call(
        functools.partial(ffn_kernel, with_pool),
        out_shape=out,
        in_specs=[SMEM] + [VMEM] * 15,
        out_specs=[VMEM] * len(out),
        scratch_shapes=[pltpu.VMEM((D, KEEP), jnp.bfloat16)] * 3
        + [pltpu.VMEM((2 * SEQ, D), jnp.bfloat16)],
        compiler_params=pltpu.CompilerParams(vmem_limit_bytes=36 << 20),
        cost_estimate=pl.CostEstimate(
            flops=2 * 3 * 2 * SEQ * D * KEEP, bytes_accessed=8 << 20, transcendentals=2 * SEQ * KEEP
        ),
        name="ffn_pool" if with_pool else "ffn",
    )(where, own0, own1, oth0, oth1, gain.reshape(2, HALF), *pieces)


def mix_kernel(where, own, oth, mix_gain, pool, pool_scale, out):
    c = where[3]
    a = own[...].astype(jnp.float32)
    b = oth[...].astype(jnp.float32)
    total = jnp.sum(a * a + b * b, axis=1, keepdims=True)
    h = (a * lax.rsqrt(total / D + EPS) * mix_gain[...]).astype(jnp.bfloat16).astype(jnp.float32)
    rows = lax.broadcasted_iota(jnp.int32, (SEQ, HALF), 0)

    def shifted(value, by):
        return jnp.where(rows >= by, pltpu.roll(value, by, 0), 0.0)

    two = h + shifted(h, 1)
    four = two + shifted(two, 2)
    eight = four + shifted(four, 4)
    wide_sum = eight + shifted(eight, 8)
    ends = rows[:, :256].astype(jnp.float32) + 1.0
    for g in range(2):
        lanes = slice(256 * g, 256 * g + 256)
        low, high = (two, eight) if g == 0 else (four, wide_sum)
        summed = jnp.where(c == 0, low[:, lanes], high[:, lanes])
        window = jnp.where(c == 0, 2.0 * (g + 1), 8.0 * (g + 1))
        pooled = summed / jnp.minimum(ends, window)
        diff = (pooled - h[:, lanes]).astype(jnp.bfloat16)
        weight = pool[:, lanes].astype(jnp.bfloat16)
        mixed = lax.dot_general(
            diff, weight, (((1,), (1,)), ((), ())), preferred_element_type=jnp.float32
        )
        out[:, lanes] = (a[:, lanes] + mixed * pool_scale[:, lanes]).astype(jnp.bfloat16)


def mix(where, own, oth, mix_gain, pool, pool_scale):
    return pl.pallas_call(
        mix_kernel,
        out_shape=jax.ShapeDtypeStruct((SEQ, HALF), jnp.bfloat16),
        in_specs=[SMEM] + [VMEM] * 5,
        out_specs=VMEM,
        compiler_params=pltpu.CompilerParams(vmem_limit_bytes=16 << 20),
        cost_estimate=pl.CostEstimate(
            flops=2 * SEQ * HALF * 256, bytes_accessed=2 << 20, transcendentals=SEQ
        ),
        name="mix",
    )(where, own, oth, mix_gain.reshape(1, HALF), pool, pool_scale.reshape(1, HALF))


def reduce_pair(base, keep, send):
    got = across(send)
    for_other = (keep[SEQ:] + got[SEQ:].astype(jnp.float32)).astype(jnp.bfloat16)
    arrived = swap(for_other, Z, 1)
    total = keep[:SEQ] + got[:SEQ].astype(jnp.float32) + arrived.astype(jnp.float32)
    return (base.astype(jnp.float32) + 0.5 * total).astype(jnp.bfloat16)


def local(tokens, pre_gain, g1, u1, d1, mix_gain, pool_weight, pool_scale, post_gain, g2, u2, d2):
    zl, y, x, c = (lax.axis_index(a) for a in ("zl", "y", "x", "c"))
    where = jnp.stack([zl, y, x, c]).astype(jnp.int32)
    own = tokens[0]
    pool = jnp.pad(
        pool_weight.transpose(2, 0, 1).reshape(POOL_ROWS, HALF), ((0, 0), (0, KEEP - HALF))
    )
    other1 = swap(pack(g1, u1, d1, 1 - zl, pool), Z, 3)
    w1 = gather(pack(g1, u1, d1, zl, pool), other1)
    mate = swap(own, Z, 1)
    own_x, mate_x = across(own), across(mate)
    keep, send, pool_all = ffn(where, own, mate, own_x, mate_x, pre_gain, w1, True)
    after_first = reduce_pair(own, keep, send)
    after_mix = mix(where, after_first, across(after_first), mix_gain, pool_all, pool_scale)
    other2 = swap(pack(g2, u2, d2, 1 - zl), Z, 3)
    w2 = gather(pack(g2, u2, d2, zl), other2)
    mate = swap(after_mix, Z, 1)
    own_x, mate_x = across(after_mix), across(mate)
    keep, send = ffn(where, after_mix, mate, own_x, mate_x, post_gain, w2, False)
    return reduce_pair(after_mix, keep, send)[None]


def solution(mesh):
    fine = Mesh(mesh.devices.reshape(2, 2, 4, 4, 2), ("zh", "zl", "y", "x", "c"))
    fs = ("zl", "y", "x")
    tokens = P(("zh",) + fs, None, "c")
    placed = (
        tokens,
        P(),
        P(fs, "c"),
        P(fs, "c"),
        P("c", fs),
        P("c"),
        P("c", None, fs),
        P("c"),
        P(),
        P(fs, "c"),
        P(fs, "c"),
        P("c", fs),
    )
    return jax.shard_map(local, mesh=fine, in_specs=placed, out_specs=tokens, check_vma=False)
```
